32 devices in a mesh: ep: 16 (over z, x, core), tp: 2 (over y).
Axes of the slice: x: 2, y: 2, z: 4, core: 2. Of those that a mesh axis runs over, the one named last changes fastest.
Arguments:
- mix_input: bfloat16 [8192, 1024], P(('ep', 'tp')), may hold values from -6 to 6
- pool_weight: bfloat16 [8, 128, 128], replicated, may hold values from -0.5 to 0.5
- pool_scale: float32 [1024], replicated, may hold values from 0.1 to 1.9
- out_weight: bfloat16 [1024, 2048], replicated, may hold values from -0.1875 to 0.1875
- moe_input: bfloat16 [2048, 2048], P('ep'), may hold values from -6 to 6
- moe_gain: float32 [2048], replicated, may hold values from 0.1 to 1.9
- group_router: bfloat16 [2048, 4], replicated, may hold values from -0.125 to 0.125
- inner_router: bfloat16 [2048, 16], replicated, may hold values from -0.125 to 0.125
- group_pick: int32 [2048], P('ep'), may hold values from 0 to 3
- inner_pick: int32 [2048, 2], P('ep'), may hold values from 0 to 3, all different within a row
- gate_weight: bfloat16 [16, 2048, 1024], P('ep', None, 'tp'), may hold values from -0.125 to 0.125
- up_weight: bfloat16 [16, 2048, 1024], P('ep', None, 'tp'), may hold values from -0.125 to 0.125
- down_weight: bfloat16 [16, 1024, 2048], P('ep', 'tp'), may hold values from -0.1875 to 0.1875
Outputs:
- mix_out: bfloat16 [8192, 2048], P(('ep', 'tp'))
- moe_out: bfloat16 [2048, 2048], P('ep', 'tp')
The draws below stay inside these ranges and needn't reach their ends.
All inputs are finite; a program needn't handle non-finite values.
Results may differ from the reference program's by a relative error of at most 0.011.
Values may be sent and summed in bfloat16 or wider, within the bound.
No kernel may reach another device: no remote copies, remote signals or barrier semaphores. Data moves between devices by JAX's collectives and lax.ppermute only.
A program may use at most 64 MiB of HBM per device.

```python
import math
import jax
import jax.numpy as jnp
import numpy as np
from jax import lax

D = 2048
FF = 1024
POOL_DIM = 128
POOL_GROUPS = 8
GROUPS = 4
TOPK = 2
WINDOW_MAX = 16
TOK_MOE = 128
D_POOL = 1024
EXPERTS = 16
EPG = 4
CAP = 32
FF_PART = 512
TOKENS_MIX = 8192
TOKENS_MOE = 2048
N_EP = 16
N_TP = 2


def touch_ends(entries, own_key, smallest, top_value):
    dims = entries.shape
    spot = [jax.random.randint(jax.random.fold_in(own_key, axis), (), 0, dims[axis]) for axis in range(len(dims))]
    entries = entries.at[tuple(spot)].set(smallest)
    longest = dims.index(max(dims))
    spot[longest] = (spot[longest] + 1) % dims[longest]
    return entries.at[tuple(spot)].set(top_value)


def shard_levels(stream_key, shape, cuts, smallest, largest):
    factor_of = 1.0
    for dim, parts in cuts:
        steps = jax.random.uniform(jax.random.fold_in(jax.random.fold_in(stream_key, 6), dim), (parts,), jnp.float32, smallest / len(cuts), largest / len(cuts))
        factor_of = factor_of * jnp.repeat(jnp.exp(steps), shape[dim] // parts).reshape((-1,) + (1,) * (len(shape) - 1 - dim))
    return factor_of


def rank_table(count, slope):
    portions = [(1 << 20) // math.isqrt(grade ** slope) + 1 for grade in range(1, count + 1)]
    deviation = 1 + sum(portions) // (1 << 30)
    return np.cumsum(np.array([max(1, weight // deviation) for weight in portions]))


def skewed_ids(stream_key, dims, amount, skew):
    table = rank_table(amount, skew)
    pick = jax.random.randint(jax.random.fold_in(stream_key, 1), dims, 0, int(table[amount - 1]))
    rank = jnp.searchsorted(jnp.asarray(table, jnp.int32), pick, side="right")
    return jax.random.permutation(jax.random.fold_in(stream_key, 2), amount)[rank].astype(jnp.int32)


def distinct(stream_key, rows, amount, top, lift):
    order = jax.random.permutation(jax.random.fold_in(stream_key, 1), amount)
    favour = order
    for power in range(3):
        favour = favour * favour // amount
    favour = favour * lift // amount
    lots = jax.random.randint(jax.random.fold_in(stream_key, 2), (rows, amount), 0, 4096) + favour
    fixed_rows = jax.random.permutation(jax.random.fold_in(stream_key, 3), rows)[jnp.arange(amount) % rows]
    lots = jnp.where(jnp.arange(rows)[:, None] == fixed_rows[None, :], 1 << 14, lots)
    score = lots * amount + jnp.arange(amount)
    return lax.top_k(score.astype(jnp.int32), top)[1].astype(jnp.int32)


def gaussian(own_key, shape, scale, limit, shards=(), held_as=jnp.bfloat16):
    entries = scale * jax.random.normal(own_key, shape, jnp.float32)
    if shards:
        entries = entries * shard_levels(own_key, shape, shards, -0.22, 0.18)
    return jnp.clip(entries, -limit, limit).astype(held_as)


def setup_inputs(seed: int = 0) -> dict:
    keys = jax.random.split(jax.random.key(seed), 14)
    mix_input = gaussian(keys[0], (TOKENS_MIX, D_POOL), 1.0, 6.0, ((0, 32),))
    pool_weight = gaussian(keys[1], (POOL_GROUPS, POOL_DIM, POOL_DIM), POOL_DIM ** -0.5, 0.5)
    pool_scale = jnp.clip(1.0 + 0.18 * jax.random.normal(keys[2], (D_POOL,), jnp.float32), 0.1, 1.9)
    out_weight = gaussian(keys[3], (D_POOL, D), D_POOL ** -0.5, 0.1875)
    moe_input = gaussian(keys[4], (TOKENS_MOE, D), 1.0, 6.0, ((0, 16),))
    moe_gain = jnp.clip(1.0 + 0.18 * jax.random.normal(keys[5], (D,), jnp.float32), 0.1, 1.9)
    group_router = gaussian(keys[6], (D, GROUPS), D ** -0.5, 0.125)
    inner_router = gaussian(keys[7], (D, EXPERTS), D ** -0.5, 0.125)
    group_pick = touch_ends(skewed_ids(keys[8], (TOKENS_MOE,), GROUPS, 2), jax.random.fold_in(keys[8], 3), 0, GROUPS - 1).astype(jnp.int32)
    inner_pick = distinct(keys[9], TOKENS_MOE, EPG, TOPK, 4096)
    gate_weight = gaussian(keys[10], (EXPERTS, D, FF), D ** -0.5, 0.125, ((0, 16), (2, 2)))
    up_weight = gaussian(keys[11], (EXPERTS, D, FF), D ** -0.5, 0.125, ((0, 16), (2, 2)))
    down_weight = gaussian(keys[12], (EXPERTS, FF, D), FF ** -0.5, 0.1875, ((0, 16), (1, 2)))
    return {"mix_input": mix_input, "pool_weight": pool_weight, "pool_scale": pool_scale, "out_weight": out_weight, "moe_input": moe_input, "moe_gain": moe_gain, "group_router": group_router, "inner_router": inner_router, "group_pick": group_pick, "inner_pick": inner_pick, "gate_weight": gate_weight, "up_weight": up_weight, "down_weight": down_weight}


NORM_FLOOR = 0.25

def trailing_means(padded, row_count, lead_rows):
    group_width = padded.shape[1] // 4
    position = jnp.arange(row_count, dtype=jnp.int32)
    pieces = []
    for scale_index in range(4):
        window = 2 ** (scale_index + 1)
        channel_block = padded[:, scale_index * group_width:(scale_index + 1) * group_width]
        window_sum = channel_block[lead_rows:lead_rows + row_count]
        for back_step in range(1, window):
            window_sum = window_sum + channel_block[lead_rows - back_step:lead_rows - back_step + row_count]
        divisor = jnp.minimum(position + 1, window).astype(jnp.float32)
        pieces.append(window_sum / divisor[:, None])
    return jnp.concatenate(pieces, axis=1)

def route_terms(group_logits, inner_logits, group_pick, inner_pick, per_group):
    group_ids = jnp.arange(group_logits.shape[1], dtype=jnp.int32)
    chosen = lax.optimization_barrier(jnp.sum(jnp.where(group_pick[:, None] == group_ids[None, :], group_logits, 0.0), axis=1))
    group_share = 1.0 / lax.optimization_barrier(jnp.sum(jnp.exp(group_logits - chosen[:, None]), axis=1))
    target = (group_pick[:, None] * per_group + inner_pick).astype(jnp.int32)
    expert_ids = jnp.arange(inner_logits.shape[1], dtype=jnp.int32)
    picked = lax.optimization_barrier(jnp.sum(jnp.where(target[:, :, None] == expert_ids[None, None, :], inner_logits[:, None, :], 0.0), axis=2))
    first_share = jax.nn.sigmoid(picked[:, 0] - picked[:, 1])
    route_weight = group_share[:, None] * jnp.stack([first_share, 1.0 - first_share], axis=1)
    return (target, route_weight)

def slot_terms(target, expert_count, capacity):
    expert_ids = jnp.arange(expert_count, dtype=jnp.int32)
    expert_hits = (target[:, :, None] == expert_ids[None, None, :]).astype(jnp.int32)
    per_token = lax.optimization_barrier(jnp.sum(expert_hits, axis=1))
    earlier = jnp.cumsum(per_token, axis=0) - per_token
    route_rank = lax.optimization_barrier(jnp.sum(expert_hits * earlier[:, None, :], axis=2))
    is_kept = route_rank < capacity
    slot_index = (target * capacity + jnp.minimum(route_rank, capacity - 1)).astype(jnp.int32)
    return (slot_index, is_kept)

def slot_sources(slot_index, is_kept, slot_count):
    token_ids = jnp.broadcast_to(jnp.arange(slot_index.shape[0], dtype=jnp.int32)[:, None], slot_index.shape)
    placed = jnp.where(is_kept, slot_index, slot_count).astype(jnp.int32).reshape(-1)
    source = jnp.zeros((slot_count,), jnp.int32).at[placed].set(token_ids.reshape(-1), mode='drop')
    slot_used = jnp.zeros((slot_count,), jnp.bool_).at[placed].set(True, mode='drop')
    return (source, slot_used)

def reference(mix_input, pool_weight, pool_scale, out_weight, moe_input, moe_gain, group_router, inner_router, group_pick, inner_pick, gate_weight, up_weight, down_weight):
    reach_back = WINDOW_MAX - 1
    row_count = mix_input.shape[0]
    values = mix_input.astype(jnp.float32)
    padded = jnp.concatenate([jnp.zeros((reach_back, values.shape[1]), jnp.float32), values], axis=0)
    trailing = trailing_means(padded, row_count, reach_back) - values
    pooled = trailing.astype(jnp.bfloat16)
    grouped = jnp.einsum('tgc,gcd->tgd', pooled.reshape(row_count, POOL_GROUPS, POOL_DIM).astype(jnp.float32), pool_weight.astype(jnp.float32))
    grouped = (grouped.reshape(row_count, D_POOL) * pool_scale[None, :]).astype(jnp.bfloat16)
    mix_out = jnp.dot(grouped, out_weight, preferred_element_type=jnp.float32).astype(jnp.bfloat16)
    token_values = moe_input.astype(jnp.float32)
    norm_scale = lax.rsqrt(jnp.maximum(lax.optimization_barrier(jnp.mean(token_values * token_values, axis=1, keepdims=True)), NORM_FLOOR))
    normed = (token_values * norm_scale * moe_gain[None, :]).astype(jnp.bfloat16)
    group_logits = jnp.dot(normed, group_router, preferred_element_type=jnp.float32)
    inner_logits = jnp.dot(normed, inner_router, preferred_element_type=jnp.float32)
    target, route_weight = route_terms(group_logits, inner_logits, group_pick, inner_pick, EPG)
    block_target = target.reshape(N_EP, TOK_MOE, TOPK)

    def block_slots(one_block):
        return slot_terms(one_block, EXPERTS, CAP)
    slot_index, is_kept = lax.map(block_slots, block_target)

    def block_sources(pair):
        return slot_sources(pair[0], pair[1], EXPERTS * CAP)
    source, slot_used = lax.map(block_sources, (slot_index, is_kept))
    global_source = source + (jnp.arange(N_EP, dtype=jnp.int32) * TOK_MOE)[:, None]
    by_expert = global_source.reshape(N_EP, EXPERTS, CAP).transpose(1, 0, 2).reshape(EXPERTS, N_EP * CAP)
    used_by_expert = slot_used.reshape(N_EP, EXPERTS, CAP).transpose(1, 0, 2).reshape(EXPERTS, N_EP * CAP)

    def run_expert(items):
        token_rows, row_used, gate_matrix, up_matrix, down_matrix = items
        expert_rows = jnp.where(row_used[:, None], normed[token_rows], jnp.zeros((), jnp.bfloat16))
        gate_sum = jnp.dot(expert_rows, gate_matrix, preferred_element_type=jnp.float32)
        up_sum = jnp.dot(expert_rows, up_matrix, preferred_element_type=jnp.float32)
        hidden = (jax.nn.silu(gate_sum) * up_sum).astype(jnp.bfloat16)
        result_sum = jnp.zeros((expert_rows.shape[0], D), jnp.float32)
        for part_index in range(N_TP):
            part_product = jnp.dot(hidden[:, part_index * FF_PART:(part_index + 1) * FF_PART], down_matrix[part_index * FF_PART:(part_index + 1) * FF_PART], preferred_element_type=jnp.float32).astype(jnp.bfloat16)
            result_sum = result_sum + lax.optimization_barrier(part_product).astype(jnp.float32)
        return result_sum.astype(jnp.bfloat16)
    results = lax.map(run_expert, (by_expert, used_by_expert, gate_weight, up_weight, down_weight))
    results = results.reshape(EXPERTS, N_EP, CAP, D)
    flat_slot = slot_index.reshape(TOKENS_MOE, TOPK)
    flat_kept = is_kept.reshape(TOKENS_MOE, TOPK)
    rank_of = (flat_slot - target * CAP).astype(jnp.int32)
    block_of = (jnp.arange(TOKENS_MOE, dtype=jnp.int32) // TOK_MOE)[:, None]
    picked = results[target, block_of, rank_of]
    route_scale = jnp.where(flat_kept, route_weight, 0.0).astype(jnp.bfloat16)
    route_scale = lax.optimization_barrier(route_scale).astype(jnp.float32)
    moe_out = lax.optimization_barrier(jnp.sum(picked.astype(jnp.float32) * route_scale[:, :, None], axis=1)).astype(jnp.bfloat16)
    return (mix_out, moe_out)
```

```python
import functools

import jax
import jax.numpy as jnp
from jax import lax
from jax.experimental import pallas as pl
from jax.experimental.pallas import tpu as pltpu
from jax.sharding import PartitionSpec as P

NORM_FLOOR = 0.25
HALO = 16
LANES = 256
SUBLANES = 8
F32 = jnp.float32
BF16 = jnp.bfloat16
I32 = jnp.int32


def call(body, name, outs, *args, scratch=(), flops=0):
    vmem = pl.BlockSpec(memory_space=pltpu.VMEM)
    smem = pl.BlockSpec(memory_space=pltpu.SMEM)
    return pl.pallas_call(
        body,
        name=name,
        out_shape=outs,
        in_specs=[smem if a.shape == (1,) else vmem for a in args],
        out_specs=jax.tree.map(lambda _: vmem, outs),
        scratch_shapes=list(scratch),
        cost_estimate=pl.CostEstimate(flops=flops, bytes_accessed=0, transcendentals=0),
    )(*args)


def dot(left, right, dims=((1,), (0,))):
    return lax.dot_general(left, right, (dims, ((), ())), preferred_element_type=F32)


def route_body(
    capacity,
    split,
    place_ref,
    x_ref,
    gain_ref,
    group_router_ref,
    inner_router_ref,
    group_pick_ref,
    inner_pick_ref,
    *rest,
):
    shared_ref, weight_ref, normed_ref = rest[0], rest[-2], rest[-1]
    tokens = x_ref.shape[0]
    groups, experts = group_router_ref.shape[0], inner_router_ref.shape[0]
    values = x_ref[...].astype(F32)
    mean = jnp.mean(values * values, axis=1, keepdims=True)
    scale = lax.rsqrt(jnp.maximum(mean, NORM_FLOOR))
    normed_ref[...] = (values * scale * gain_ref[...]).astype(BF16)

    normed = normed_ref[...]
    group_logits = dot(group_router_ref[...], normed, ((1,), (1,)))
    inner_logits = dot(inner_router_ref[...], normed, ((1,), (1,)))
    group_pick = group_pick_ref[...]
    group_row = lax.broadcasted_iota(I32, (groups, tokens), 0)
    chosen = jnp.sum(
        jnp.where(group_row == group_pick, group_logits, 0.0), axis=0, keepdims=True
    )
    share = 1.0 / jnp.sum(jnp.exp(group_logits - chosen), axis=0, keepdims=True)
    expert_row = lax.broadcasted_iota(I32, (experts, tokens), 0)
    base = group_pick * (experts // groups)
    first = expert_row == base + inner_pick_ref[0:1, :]
    second = expert_row == base + inner_pick_ref[1:2, :]
    first_logit = jnp.sum(jnp.where(first, inner_logits, 0.0), axis=0, keepdims=True)
    second_logit = jnp.sum(jnp.where(second, inner_logits, 0.0), axis=0, keepdims=True)
    pair = 1.0 / (1.0 + jnp.exp(second_logit - first_logit))
    route = jnp.where(first, share * pair, jnp.where(second, share * (1.0 - pair), 0.0))

    hits = jnp.where(first | second, 1.0, 0.0)
    row = lax.broadcasted_iota(I32, (tokens, tokens), 0)
    col = lax.broadcasted_iota(I32, (tokens, tokens), 1)
    before = jnp.where(row < col, 1.0, 0.0).astype(BF16)
    rank = dot(hits.astype(BF16), before)
    rank = jnp.where(hits > 0.0, rank, float(tokens)).astype(I32)

    slot = lax.broadcasted_iota(I32, (capacity, tokens), 0)
    shared, direct = [], []
    for e in range(experts):
        is_here = slot == rank[e : e + 1, :]
        weight_ref[e * capacity : (e + 1) * capacity, :] = jnp.where(
            is_here, route[e : e + 1, :], 0.0
        ).astype(BF16)
        picked = jnp.where(is_here, 1.0, 0.0)
        shared.append(picked[:split])
        direct.append(picked[split:])
    width = shared_ref.shape[1]
    start = pl.multiple_of(place_ref[0] * width, width)
    shared = jnp.concatenate(shared, axis=0).astype(BF16)
    shared_ref[...] = dot(shared, normed_ref[:, pl.ds(start, width)]).astype(BF16)
    if split < capacity:
        direct = jnp.concatenate(direct, axis=0).astype(BF16)
        rest[1][...] = dot(direct, normed).astype(BF16)


def up_body(shares, has_direct, place_ref, *refs):
    shared_refs, refs = refs[:shares], refs[shares:]
    direct_refs, refs = (refs[:1], refs[1:]) if has_direct else ((), refs)
    gate_ref, up_ref, hidden_ref = refs
    rows, width = shared_refs[0].shape
    place = place_ref[0]
    columns = min(LANES, hidden_ref.shape[1])
    for n in range(0, hidden_ref.shape[1], columns):
        part = slice(n, n + columns)
        gate = up = None
        for shift, ref in enumerate(shared_refs):
            owner = lax.rem(place - shift + shares, shares)
            span = pl.ds(pl.multiple_of(owner * width, width), width)
            g = dot(ref[...], gate_ref[0, span, part])
            u = dot(ref[...], up_ref[0, span, part])
            gate, up = (g, u) if gate is None else (gate + g, up + u)
        hidden_ref[:rows, part] = (gate / (1.0 + jnp.exp(-gate)) * up).astype(BF16)
        for ref in direct_refs:
            gate = dot(ref[...], gate_ref[0, :, part])
            up = dot(ref[...], up_ref[0, :, part])
            hidden_ref[rows:, part] = (gate / (1.0 + jnp.exp(-gate)) * up).astype(BF16)


def down_body(shares, split, place_ref, *refs):
    hidden_refs, (down_ref, *sent_refs), out_ref = refs[:shares], refs[shares:-1], refs[-1]
    sources, capacity, width = out_ref.shape
    shared_rows = sources * split
    start = pl.multiple_of(place_ref[0] * width, width)
    columns = min(LANES, width)
    for n in range(0, width, columns):
        part = slice(n, n + columns)
        own = pl.ds(pl.multiple_of(start + n, columns), columns)
        total = dot(hidden_refs[0][...], down_ref[0, :, own])
        for hidden_ref, sent_ref in zip(hidden_refs[1:], sent_refs):
            total = total + dot(hidden_ref[...], sent_ref[:, part])
        total = total.astype(BF16)
        out_ref[:, :split, part] = total[:shared_rows].reshape(sources, split, columns)
        if split < capacity:
            out_ref[:, split:, part] = total[shared_rows:].reshape(
                sources, capacity - split, columns
            )


def combine_body(weight_ref, result_ref, out_ref):
    out_ref[...] = dot(weight_ref[...], result_ref[...], ((0,), (0,))).astype(BF16)


def mixer_body(
    place_ref, before_ref, x_ref, pool_ref, pool_scale_ref, out_weight_ref, out_ref, grouped_ref
):
    rows, width = x_ref.shape
    groups, group_dim = pool_ref.shape[0], pool_ref.shape[1]
    position = place_ref[0] * rows + lax.broadcasted_iota(I32, (rows, 1), 0)
    span = width // 4
    for scale_index in range(4):
        window = 2 ** (scale_index + 1)
        part = slice(scale_index * span, (scale_index + 1) * span)
        total = jnp.concatenate([before_ref[:, part], x_ref[:, part]], axis=0).astype(F32)
        values = total[HALO:]
        step = 1
        while step < window:
            total = total + pltpu.roll(total, step, 0)
            step *= 2
        share = 1.0 / jnp.minimum(position + 1, window).astype(F32)
        pooled = (total[HALO:] * share - values).astype(BF16)
        for inner in range(span // group_dim):
            group = scale_index * (span // group_dim) + inner
            lanes = slice(group * group_dim, (group + 1) * group_dim)
            product = dot(pooled[:, inner * group_dim : (inner + 1) * group_dim], pool_ref[group])
            grouped_ref[:, lanes] = (product * pool_scale_ref[:, lanes]).astype(BF16)
    grouped = grouped_ref[...]
    for n in range(0, out_ref.shape[1], 2 * LANES):
        part = slice(n, n + 2 * LANES)
        out_ref[:, part] = dot(grouped, out_weight_ref[:, part]).astype(BF16)


def shifted(value, axis, steps, count):
    return lax.ppermute(value, axis, [(s, (s + steps) % count) for s in range(count)])


def per_device(
    mix_input,
    pool_weight,
    pool_scale,
    out_weight,
    moe_input,
    moe_gain,
    group_router,
    inner_router,
    group_pick,
    inner_pick,
    gate_weight,
    up_weight,
    down_weight,
):
    shares = lax.axis_size("tp")
    ranks = lax.axis_size("ep")
    place = lax.axis_index("tp").astype(I32)
    here = place.reshape(1)

    tokens, features = moe_input.shape
    experts = inner_router.shape[1]
    capacity = 2 * inner_pick.shape[1] * tokens // experts
    split = capacity
    if capacity >= 2 * SUBLANES:
        split = 3 * capacity // 4 // SUBLANES * SUBLANES
    direct = capacity - split
    width = features // shares
    units = down_weight.shape[1]

    sent_down = []
    for shift in range(1, shares):
        target = lax.rem(place + shift, shares)
        block = lax.dynamic_slice(down_weight[0], (0, target * width), (units, width))
        sent_down.append(shifted(block, "tp", shift, shares))

    shapes = [jax.ShapeDtypeStruct((experts * split, width), BF16)]
    if direct:
        shapes.append(jax.ShapeDtypeStruct((experts * direct, features), BF16))
    shapes.append(jax.ShapeDtypeStruct((experts * capacity, tokens), BF16))
    *outgoing, route_weight = call(
        functools.partial(route_body, capacity, split),
        "route",
        shapes,
        here,
        moe_input,
        moe_gain.reshape(1, -1),
        group_router.T,
        inner_router.T,
        group_pick.reshape(1, -1),
        inner_pick.T,
        scratch=[pltpu.VMEM((tokens, features), BF16)],
        flops=2 * experts * capacity * tokens * features,
    )

    arrived = [lax.all_to_all(o, "ep", split_axis=0, concat_axis=0, tiled=True) for o in outgoing]
    shared = [arrived[0]]
    for shift in range(1, shares):
        shared.append(shifted(arrived[0], "tp", shift, shares))
    rows = ranks * capacity
    hidden = call(
        functools.partial(up_body, shares, direct > 0),
        "up",
        jax.ShapeDtypeStruct((rows, units), BF16),
        here,
        *shared,
        *arrived[1:],
        gate_weight,
        up_weight,
        flops=4 * rows * features * units,
    )
    hiddens = [hidden]
    for shift in range(1, shares):
        hiddens.append(shifted(hidden, "tp", shift, shares))
    result = call(
        functools.partial(down_body, shares, split),
        "down",
        jax.ShapeDtypeStruct((ranks, capacity, width), BF16),
        here,
        *hiddens,
        down_weight,
        *sent_down,
        flops=2 * rows * units * shares * width,
    )
    returned = lax.all_to_all(result, "ep", split_axis=0, concat_axis=0, tiled=True)
    moe_out = call(
        combine_body,
        "combine",
        jax.ShapeDtypeStruct((tokens, width), BF16),
        route_weight,
        returned.reshape(experts * capacity, width),
        flops=2 * rows * tokens * width,
    )

    row_count, pool_width = mix_input.shape
    count = ranks * shares
    before = lax.ppermute(
        mix_input[row_count - HALO :], ("ep", "tp"), [(s, s + 1) for s in range(count - 1)]
    )
    seat = (lax.axis_index("ep") * shares + place).astype(I32).reshape(1)
    mix_out = call(
        mixer_body,
        "mixer",
        jax.ShapeDtypeStruct((row_count, out_weight.shape[1]), BF16),
        seat,
        before,
        mix_input,
        pool_weight,
        pool_scale.reshape(1, -1),
        out_weight,
        scratch=[pltpu.VMEM((row_count, pool_width), BF16)],
        flops=2 * row_count * pool_width * out_weight.shape[1],
    )
    return (mix_out, moe_out)


def solution(mesh):
    in_specs = (
        P(("ep", "tp"), None),
        P(),
        P(),
        P(),
        P("ep", None),
        P(),
        P(),
        P(),
        P("ep"),
        P("ep", None),
        P("ep", None, "tp"),
        P("ep", None, "tp"),
        P("ep", "tp", None),
    )
    out_specs = (P(("ep", "tp"), None), P("ep", "tp"))
    return jax.shard_map(
        per_device, mesh=mesh, in_specs=in_specs, out_specs=out_specs, check_vma=False
    )
```
